32 devices in a mesh: rep: 2 (over x), fs: 8 (over z, y), tp: 2 (over core).
Axes of the slice: x: 2, y: 2, z: 4, core: 2. Of those that a mesh axis runs over, the one named last changes fastest.
Arguments:
- activations: bfloat16 [3072, 2048], P(('rep', 'fs'), 'tp'), may hold values from -6 to 6
- mix_gain: float32 [2048], replicated, may hold values from 0.1 to 1.9
- mlp_gain: float32 [2048], replicated, may hold values from 0.1 to 1.9
- query_weight: float32 [2048, 512], P('fs', 'tp'), may hold values from -0.125 to 0.125
- query_scale: float32 [512], P('tp'), may hold values from 0.3 to 3
- key_weight: float32 [2048, 512], P('fs', 'tp'), may hold values from -0.125 to 0.125
- key_scale: float32 [512], P('tp'), may hold values from 0.3 to 3
- value_weight: float32 [2048, 1024], P('fs', 'tp'), may hold values from -0.125 to 0.125
- value_scale: float32 [1024], P('tp'), may hold values from 0.3 to 3
- gate_weight: float32 [2048, 1024], P('fs', 'tp'), may hold values from -0.125 to 0.125
- gate_scale: float32 [1024], P('tp'), may hold values from 0.3 to 3
- out_weight: float32 [1024, 2048], P('tp', 'fs'), may hold values from -0.1875 to 0.1875
- out_scale: float32 [2048], P('fs'), may hold values from 0.3 to 3
- up_weight: float32 [2048, 8192], P('fs', 'tp'), may hold values from -0.125 to 0.125
- up_scale: float32 [8192], P('tp'), may hold values from 0.3 to 3
- down_weight: float32 [8192, 2048], P('tp', 'fs'), may hold values from -0.0625 to 0.0625
- down_scale: float32 [2048], P('fs'), may hold values from 0.3 to 3
- log_decay: float32 [8], P('tp'), may hold values from -0.1 to 0, as said below
Outputs:
- result: bfloat16 [3072, 2048], P(('rep', 'fs'), 'tp')
The draws below stay inside these ranges and needn't reach their ends.
Inputs may be any that keep to these rules, and one draw needn't show every extreme that they name: `log_decay`: negative for every head.
All inputs are finite; a program needn't handle non-finite values.
Results may differ from the reference program's by a relative error of at most 0.023.
Values may be sent and summed in bfloat16 or wider, within the bound.
A program may use at most 128 MiB of HBM per device.

```python
import math
import jax
import jax.numpy as jnp
from jax import lax

D = 2048
HEADS = 8
QK = 64
VD = 128
FF = 8192
BLOCK = 64
LENGTH = 192
QK_WIDTH = 512
V_WIDTH = 1024
ROWS = 3072
N_TP = 2


def draw_log_decay(key, part):
    order = jax.random.permutation(jax.random.fold_in(key, 11), HEADS)
    quick = order < HEADS // 2
    slow_rate = jax.random.uniform(jax.random.fold_in(key, 12), (HEADS,), jnp.float32, 0.1, 2.0) / LENGTH
    quick_rate = jax.random.uniform(jax.random.fold_in(key, 13), (HEADS,), jnp.float32, 0.04, 0.1)
    chosen = -jnp.where(quick, quick_rate, slow_rate)
    return chosen.astype(jnp.float32)


def steps_of(stream_key, extent, split, least, high):
    def one(position, shards_of):
        draws = jax.random.uniform(jax.random.fold_in(jax.random.fold_in(stream_key, 6), position), (shards_of,), jnp.float32, least / len(split), high / len(split))
        return jnp.repeat(jnp.exp(draws), extent[position] // shards_of).reshape((-1,) + (1,) * (len(extent) - position - 1))

    level = one(*split[0])
    for cut in split[1:]:
        level = level * one(*cut)
    return level


def centred(stream_key, shape, spread, limit, pieces=(), kind=jnp.bfloat16):
    loudness = steps_of(stream_key, shape, pieces, -0.22, 0.18) if pieces else 1.0
    result = jax.random.normal(stream_key, shape, jnp.float32) * spread * loudness
    return jnp.minimum(jnp.maximum(result, -limit), limit).astype(kind)


def setup_inputs(seed: int = 0) -> dict:
    key_list = jax.random.split(jax.random.key(seed), 19)
    return {
        "activations": centred(key_list[0], (ROWS, D), 1.0, 6.0, ((0, 16), (1, 2))),
        "mix_gain": jnp.clip(1.0 + 0.18 * jax.random.normal(key_list[1], (D,), jnp.float32), 0.1, 1.9),
        "mlp_gain": jnp.clip(1.0 + 0.18 * jax.random.normal(key_list[2], (D,), jnp.float32), 0.1, 1.9),
        "query_weight": centred(key_list[3], (D, QK_WIDTH), D ** -0.5, 0.125, ((0, 8), (1, 2)), jnp.float32),
        "query_scale": jnp.clip(jnp.exp(math.log(3.0) - 2.3025851 * jax.random.uniform(key_list[4], (QK_WIDTH,), jnp.float32) ** steps_of(key_list[4], (QK_WIDTH,), ((0, 2),), -0.2, 0.2)), 0.3, 3.0),
        "key_weight": centred(key_list[5], (D, QK_WIDTH), D ** -0.5, 0.125, ((0, 8), (1, 2)), jnp.float32),
        "key_scale": jnp.clip(jnp.exp(math.log(3.0) - 2.3025851 * jax.random.uniform(key_list[6], (QK_WIDTH,), jnp.float32) ** steps_of(key_list[6], (QK_WIDTH,), ((0, 2),), -0.2, 0.2)), 0.3, 3.0),
        "value_weight": centred(key_list[7], (D, V_WIDTH), D ** -0.5, 0.125, ((0, 8), (1, 2)), jnp.float32),
        "value_scale": jnp.clip(jnp.exp(math.log(3.0) - 2.3025851 * jax.random.uniform(key_list[8], (V_WIDTH,), jnp.float32) ** steps_of(key_list[8], (V_WIDTH,), ((0, 2),), -0.2, 0.2)), 0.3, 3.0),
        "gate_weight": centred(key_list[9], (D, V_WIDTH), D ** -0.5, 0.125, ((0, 8), (1, 2)), jnp.float32),
        "gate_scale": jnp.clip(jnp.exp(math.log(3.0) - 2.3025851 * jax.random.uniform(key_list[10], (V_WIDTH,), jnp.float32) ** steps_of(key_list[10], (V_WIDTH,), ((0, 2),), -0.2, 0.2)), 0.3, 3.0),
        "out_weight": centred(key_list[11], (V_WIDTH, D), V_WIDTH ** -0.5, 0.1875, ((0, 2), (1, 8)), jnp.float32),
        "out_scale": jnp.clip(jnp.exp(math.log(3.0) - 2.3025851 * jax.random.uniform(key_list[12], (D,), jnp.float32) ** steps_of(key_list[12], (D,), ((0, 8),), -0.2, 0.2)), 0.3, 3.0),
        "up_weight": centred(key_list[13], (D, FF), D ** -0.5, 0.125, ((0, 8), (1, 2)), jnp.float32),
        "up_scale": jnp.clip(jnp.exp(math.log(3.0) - 2.3025851 * jax.random.uniform(key_list[14], (FF,), jnp.float32) ** steps_of(key_list[14], (FF,), ((0, 2),), -0.2, 0.2)), 0.3, 3.0),
        "down_weight": centred(key_list[15], (FF, D), FF ** -0.5, 0.0625, ((0, 2), (1, 8)), jnp.float32),
        "down_scale": jnp.clip(jnp.exp(math.log(3.0) - 2.3025851 * jax.random.uniform(key_list[16], (D,), jnp.float32) ** steps_of(key_list[16], (D,), ((0, 8),), -0.2, 0.2)), 0.3, 3.0),
        "log_decay": draw_log_decay(jax.random.fold_in(key_list[18], 71), 0),
    }


epsilon = 1e-06
rope_base = 10000.0

def normalize(rows, gain):
    wide = rows.astype(jnp.float32)
    mean_square = lax.optimization_barrier(jnp.mean(wide * wide, axis=-1, keepdims=True))
    return (wide * lax.rsqrt(mean_square + epsilon) * gain).astype(jnp.bfloat16)

def rotate(head_rows, positions):
    half = head_rows.shape[-1] // 2
    inverse = 1.0 / rope_base ** jnp.linspace(0.0, 1.0, half, dtype=jnp.float32)
    angles = positions[:, None] * inverse[None, :]
    cosine = jnp.cos(angles)[:, None, :]
    sine = jnp.sin(angles)[:, None, :]
    first = head_rows[..., :half]
    second = head_rows[..., half:]
    return jnp.concatenate([first * cosine - second * sine, first * sine + second * cosine], axis=-1)

def retain(query_heads, key_heads, value_heads, log_decay):
    batch, length, heads, width = query_heads.shape
    block_count = length // BLOCK
    highest = lax.Precision.HIGHEST

    def to_blocks(tensor):
        return tensor.reshape(batch, block_count, BLOCK, heads, tensor.shape[-1]).transpose(0, 3, 1, 2, 4)
    query_blocks = to_blocks(query_heads)
    key_blocks = to_blocks(key_heads)
    value_blocks = to_blocks(value_heads)
    places = jnp.arange(BLOCK, dtype=jnp.float32)
    offsets = places[:, None] - places[None, :]
    inner = jnp.where(offsets >= 0, jnp.exp(log_decay[:, None, None] * jnp.maximum(offsets, 0.0)), 0.0)
    scores = jnp.einsum('bhntd,bhnsd->bhnts', query_blocks, key_blocks, precision=highest) * inner[None, :, None]
    output = jnp.einsum('bhnts,bhnse->bhnte', scores, value_blocks, precision=highest)
    keys_decayed = key_blocks * jnp.exp(log_decay[:, None] * (BLOCK - 1.0 - places)[None, :])[None, :, None, :, None]
    increments = jnp.einsum('bhnsd,bhnse->nbhde', keys_decayed, value_blocks, precision=highest)
    carry_decay = jnp.exp(log_decay * BLOCK)[None, :, None, None]

    def advance(state, increment):
        return (carry_decay * state + increment, state)
    initial = jnp.zeros((batch, heads, width, value_heads.shape[-1]), jnp.float32)
    _, states = lax.scan(advance, initial, increments)
    query_decayed = query_blocks * jnp.exp(log_decay[:, None] * (places + 1.0)[None, :])[None, :, None, :, None]
    output = output + jnp.einsum('bhntd,nbhde->bhnte', query_decayed, states, precision=highest)
    return output.transpose(0, 2, 3, 1, 4).reshape(batch, length, heads, value_heads.shape[-1])

def split_sum(rows, weight, scale):
    width = rows.shape[1] // N_TP
    weight_half = weight.astype(jnp.bfloat16)
    total = jnp.zeros((rows.shape[0], weight.shape[1]), jnp.float32)
    for group in range(N_TP):
        partial_value = jnp.dot(rows[:, group * width:(group + 1) * width], weight_half[group * width:(group + 1) * width], preferred_element_type=jnp.float32) * scale
        rounded = lax.optimization_barrier(partial_value.astype(jnp.bfloat16))
        total = total + rounded.astype(jnp.float32)
    return total

def reference(activations, mix_gain, mlp_gain, query_weight, query_scale, key_weight, key_scale, value_weight, value_scale, gate_weight, gate_scale, out_weight, out_scale, up_weight, up_scale, down_weight, down_scale, log_decay):
    normed = normalize(activations, mix_gain)

    def project(weight, scale):
        return jnp.dot(normed, weight.astype(jnp.bfloat16), preferred_element_type=jnp.float32) * scale
    query = project(query_weight, query_scale)
    key_rows = project(key_weight, key_scale)
    value = project(value_weight, value_scale)
    gate = project(gate_weight, gate_scale)
    total_rows = activations.shape[0]
    sequences = total_rows // LENGTH
    positions = jnp.arange(LENGTH, dtype=jnp.float32)
    query_heads = rotate(query.reshape(sequences, LENGTH, HEADS, QK), positions)
    key_heads = rotate(key_rows.reshape(sequences, LENGTH, HEADS, QK), positions)
    value_heads = value.reshape(sequences, LENGTH, HEADS, VD)
    retained = retain(query_heads, key_heads, value_heads, log_decay)
    retained = retained * lax.rsqrt(lax.optimization_barrier(jnp.mean(retained * retained, axis=-1, keepdims=True)) + epsilon)
    attended = (retained.reshape(total_rows, V_WIDTH) * jax.nn.silu(gate)).astype(jnp.bfloat16)
    mixed = split_sum(attended, out_weight, out_scale)
    first = (activations.astype(jnp.float32) + mixed).astype(jnp.bfloat16)
    normed_two = normalize(first, mlp_gain)
    raised = jnp.dot(normed_two, up_weight.astype(jnp.bfloat16), preferred_element_type=jnp.float32) * up_scale
    hidden = jnp.square(jax.nn.relu(raised)).astype(jnp.bfloat16)
    channel = split_sum(hidden, down_weight, down_scale)
    return (first.astype(jnp.float32) + channel).astype(jnp.bfloat16)
```

```python
import jax
import jax.numpy as jnp
from jax import lax
from jax.sharding import PartitionSpec as P

BLOCK = 64
LENGTH = 192


epsilon = 1e-06
rope_base = 10000.0


def rotate(head_rows, positions):
    half = head_rows.shape[-1] // 2
    inverse = 1.0 / rope_base ** jnp.linspace(0.0, 1.0, half, dtype=jnp.float32)
    angles = positions[:, None] * inverse[None, :]
    cosine = jnp.cos(angles)[:, None, :]
    sine = jnp.sin(angles)[:, None, :]
    first = head_rows[..., :half]
    second = head_rows[..., half:]
    return jnp.concatenate(
        [first * cosine - second * sine, first * sine + second * cosine], axis=-1
    )


def retain(query_heads, key_heads, value_heads, log_decay):
    batch, length, heads, width = query_heads.shape
    block_count = length // BLOCK
    highest = lax.Precision.HIGHEST

    def to_blocks(tensor):
        return tensor.reshape(batch, block_count, BLOCK, heads, tensor.shape[-1]).transpose(
            0, 3, 1, 2, 4
        )

    query_blocks = to_blocks(query_heads)
    key_blocks = to_blocks(key_heads)
    value_blocks = to_blocks(value_heads)
    places = jnp.arange(BLOCK, dtype=jnp.float32)
    offsets = places[:, None] - places[None, :]
    inner = jnp.where(
        offsets >= 0, jnp.exp(log_decay[:, None, None] * jnp.maximum(offsets, 0.0)), 0.0
    )
    scores = (
        jnp.einsum("bhntd,bhnsd->bhnts", query_blocks, key_blocks, precision=highest)
        * inner[None, :, None]
    )
    output = jnp.einsum("bhnts,bhnse->bhnte", scores, value_blocks, precision=highest)
    keys_decayed = (
        key_blocks
        * jnp.exp(log_decay[:, None] * (BLOCK - 1.0 - places)[None, :])[None, :, None, :, None]
    )
    increments = jnp.einsum("bhnsd,bhnse->nbhde", keys_decayed, value_blocks, precision=highest)
    carry_decay = jnp.exp(log_decay * BLOCK)[None, :, None, None]

    def advance(state, increment):
        return (carry_decay * state + increment, state)

    initial = jnp.zeros((batch, heads, width, value_heads.shape[-1]), jnp.float32)
    _, states = lax.scan(advance, initial, increments)
    query_decayed = (
        query_blocks * jnp.exp(log_decay[:, None] * (places + 1.0)[None, :])[None, :, None, :, None]
    )
    output = output + jnp.einsum("bhntd,nbhde->bhnte", query_decayed, states, precision=highest)
    return output.transpose(0, 2, 3, 1, 4).reshape(batch, length, heads, value_heads.shape[-1])


def norm_half(rows, gain):
    wide = rows.astype(jnp.float32)
    total = lax.psum(jnp.sum(wide * wide, axis=1, keepdims=True), "tp")
    width = rows.shape[1]
    parts = lax.axis_size("tp")
    mine = lax.dynamic_slice(gain, (lax.axis_index("tp") * width,), (width,))
    scaled = wide * lax.rsqrt(total / (width * parts) + epsilon) * mine
    return scaled.astype(jnp.bfloat16)


def tp_columns(rows):
    return lax.all_gather(rows, "tp", axis=1, tiled=True)


def heads_of(normed, weight, scale):
    return jnp.dot(normed, weight, preferred_element_type=jnp.float32) * scale


def mixer(activations, mix_gain, four, four_scale, out_full, out_columns, log_decay):
    normed = tp_columns(norm_half(activations, mix_gain))
    total_rows = normed.shape[0]
    sequences = total_rows // LENGTH
    heads = log_decay.shape[0]
    joined = heads_of(normed, four, four_scale)
    unit = joined.shape[1] // 6
    query = joined[:, :unit]
    key_rows = joined[:, unit : 2 * unit]
    value = joined[:, 2 * unit : 4 * unit]
    gate = joined[:, 4 * unit :]
    positions = jnp.arange(LENGTH, dtype=jnp.float32)
    query_heads = rotate(query.reshape(sequences, LENGTH, heads, -1), positions)
    key_heads = rotate(key_rows.reshape(sequences, LENGTH, heads, -1), positions)
    value_heads = value.reshape(sequences, LENGTH, heads, -1)
    retained = retain(query_heads, key_heads, value_heads, log_decay)
    retained = retained * lax.rsqrt(jnp.mean(retained * retained, axis=-1, keepdims=True) + epsilon)
    attended = (retained.reshape(total_rows, -1) * jax.nn.silu(gate)).astype(jnp.bfloat16)
    partial_value = jnp.einsum(
        "rk,jkc->rjc", attended, out_full, preferred_element_type=jnp.float32
    ).reshape(total_rows, -1)
    partial_value = (partial_value * out_columns).astype(jnp.bfloat16)
    mixed = tp_sum(partial_value)
    return (activations.astype(jnp.float32) + mixed).astype(jnp.bfloat16)


def tp_sum(partial_value):
    parts = lax.axis_size("tp")
    width = partial_value.shape[1] // parts
    spread = jnp.moveaxis(partial_value.reshape(-1, parts, width), 1, 0)
    arrived = lax.all_to_all(spread, "tp", 0, 0, tiled=True)
    return jnp.sum(arrived.astype(jnp.float32), axis=0)


def on_device(
    activations,
    mix_gain,
    mlp_gain,
    query_weight,
    query_scale,
    key_weight,
    key_scale,
    value_weight,
    value_scale,
    gate_weight,
    gate_scale,
    out_weight,
    out_scale,
    up_weight,
    up_scale,
    down_weight,
    down_scale,
    log_decay,
):
    bf = jnp.bfloat16
    four_weight = jnp.concatenate(
        [query_weight, key_weight, value_weight, gate_weight], axis=1
    ).astype(bf)
    four_scale = jnp.concatenate([query_scale, key_scale, value_scale, gate_scale])
    four = lax.all_gather(four_weight, "fs", axis=0, tiled=True)
    out_full = lax.all_gather(out_weight.astype(bf), "fs", axis=0)
    scales = lax.all_gather(jnp.stack([out_scale, down_scale]), "fs", axis=1, tiled=True)
    up_mine = lax.all_to_all(up_weight.astype(bf), "fs", 1, 0, tiled=True)
    down_mine = lax.all_to_all(down_weight.astype(bf), "fs", 0, 1, tiled=True)
    units = up_mine.shape[1]
    up_columns = lax.dynamic_slice(up_scale, (lax.axis_index("fs") * units,), (units,))
    first = mixer(activations, mix_gain, four, four_scale, out_full, scales[0], log_decay)
    half_rows = norm_half(first, mlp_gain)
    normed_two = tp_columns(lax.all_gather(half_rows, "fs", axis=0, tiled=True))
    raised = jnp.dot(normed_two, up_mine, preferred_element_type=jnp.float32) * up_columns
    hidden = jnp.square(jax.nn.relu(raised)).astype(bf)
    share = jnp.dot(hidden, down_mine, preferred_element_type=jnp.float32) * scales[1]
    pair = tp_sum(share.astype(bf)).astype(bf)
    arrived = lax.all_to_all(
        pair.reshape(-1, first.shape[0], first.shape[1]), "fs", 0, 0, tiled=True
    )
    channel = jnp.sum(arrived.astype(jnp.float32), axis=0)
    return (first.astype(jnp.float32) + channel).astype(bf)


def solution(mesh):
    placed = (
        P(("rep", "fs"), "tp"),
        P(),
        P(),
        P("fs", "tp"),
        P("tp"),
        P("fs", "tp"),
        P("tp"),
        P("fs", "tp"),
        P("tp"),
        P("fs", "tp"),
        P("tp"),
        P("tp", "fs"),
        P("fs"),
        P("fs", "tp"),
        P("tp"),
        P("tp", "fs"),
        P("fs"),
        P("tp"),
    )
    return jax.shard_map(
        on_device, mesh=mesh, in_specs=placed, out_specs=P(("rep", "fs"), "tp"), check_vma=False
    )
```

```python
import functools

import jax
import jax.numpy as jnp
from jax import lax
from jax.experimental import pallas as pl
from jax.experimental.pallas import tpu as pltpu
from jax.sharding import PartitionSpec as P

BLOCK = 64
LENGTH = 192


epsilon = 1e-06
rope_base = 10000.0


def rotate(head_rows, positions):
    half = head_rows.shape[-1] // 2
    inverse = 1.0 / rope_base ** jnp.linspace(0.0, 1.0, half, dtype=jnp.float32)
    angles = positions[:, None] * inverse[None, :]
    cosine = jnp.cos(angles)[:, None, :]
    sine = jnp.sin(angles)[:, None, :]
    first = head_rows[..., :half]
    second = head_rows[..., half:]
    return jnp.concatenate(
        [first * cosine - second * sine, first * sine + second * cosine], axis=-1
    )


def retain(query_heads, key_heads, value_heads, log_decay):
    batch, length, heads, width = query_heads.shape
    block_count = length // BLOCK
    highest = lax.Precision.HIGHEST

    def to_blocks(tensor):
        return tensor.reshape(batch, block_count, BLOCK, heads, tensor.shape[-1]).transpose(
            0, 3, 1, 2, 4
        )

    query_blocks = to_blocks(query_heads)
    key_blocks = to_blocks(key_heads)
    value_blocks = to_blocks(value_heads)
    places = jnp.arange(BLOCK, dtype=jnp.float32)
    offsets = places[:, None] - places[None, :]
    inner = jnp.where(
        offsets >= 0, jnp.exp(log_decay[:, None, None] * jnp.maximum(offsets, 0.0)), 0.0
    )
    scores = (
        jnp.einsum("bhntd,bhnsd->bhnts", query_blocks, key_blocks, precision=highest)
        * inner[None, :, None]
    )
    output = jnp.einsum("bhnts,bhnse->bhnte", scores, value_blocks, precision=highest)
    keys_decayed = (
        key_blocks
        * jnp.exp(log_decay[:, None] * (BLOCK - 1.0 - places)[None, :])[None, :, None, :, None]
    )
    increments = jnp.einsum("bhnsd,bhnse->nbhde", keys_decayed, value_blocks, precision=highest)
    carry_decay = jnp.exp(log_decay * BLOCK)[None, :, None, None]

    def advance(state, increment):
        return (carry_decay * state + increment, state)

    initial = jnp.zeros((batch, heads, width, value_heads.shape[-1]), jnp.float32)
    _, states = lax.scan(advance, initial, increments)
    query_decayed = (
        query_blocks * jnp.exp(log_decay[:, None] * (places + 1.0)[None, :])[None, :, None, :, None]
    )
    output = output + jnp.einsum("bhntd,nbhde->bhnte", query_decayed, states, precision=highest)
    return output.transpose(0, 2, 3, 1, 4).reshape(batch, length, heads, value_heads.shape[-1])


MESH = pl.DeviceIdType.MESH


def ring_place(index, n):
    odd = index % 2
    return (1 - odd) * (index // 2) + odd * (n - 1 - index // 2)


def ring_index(place, n):
    place = (place + n) % n
    late = (2 * place) // n
    return (1 - late) * (2 * place) + late * (2 * (n - 1 - place) + 1)


def greet(targets):
    barrier = pltpu.get_barrier_semaphore()
    for target in targets:
        pl.semaphore_signal(barrier, inc=1, device_id=target, device_id_type=MESH)
    pl.semaphore_wait(barrier, len(targets))


def remote(source, target, send, recv, device):
    return pltpu.make_async_remote_copy(
        src_ref=source,
        dst_ref=target,
        send_sem=send,
        recv_sem=recv,
        device_id=device,
        device_id_type=MESH,
    )


def ring_gather_kernel(n, count, shared, *refs):
    ins, outs = refs[:count], refs[count : 2 * count]
    own_sem, send_sem, recv_sem, xsend_sem, xrecv_sem = refs[2 * count :]
    me = lax.axis_index("fs")
    place = ring_place(me, n)
    chunks = ins[0].shape[0]
    quarter = chunks // 4
    right = {"fs": ring_index(place + 1, n)}
    left = {"fs": ring_index(place + n - 1, n)}
    targets = [right, left]
    if shared:
        rep = lax.axis_index("rep")
        across = {"rep": 1 - rep}
        targets.append(across)
        lanes = [
            (rep * 2, 1, 0),
            (rep * 2 + 1, -1, 1),
            (4, 1, None),
            (6, -1, None),
            (5, 1, None),
            (7, -1, None),
        ]
    else:
        lanes = [(k, 1 if k % 2 == 0 else -1, None) for k in range(chunks)]
    greet(targets)
    owns = [
        pltpu.make_async_copy(ins[a], outs[a].at[me], own_sem.at[a]) for a in range(count)
    ]
    for own in owns:
        own.start()
    for k, (chunk, way, _) in enumerate(lanes):
        for a in range(count):
            remote(
                ins[a].at[chunk],
                outs[a].at[me, chunk],
                send_sem.at[a, k],
                recv_sem.at[0, a, k],
                right if way == 1 else left,
            ).start()

    def step(s, _):
        for k, (chunk, way, extra) in enumerate(lanes):
            owner = ring_index(place + (n - s if way == 1 else s), n)
            for a in range(count):
                block = outs[a].at[owner, chunk]
                device = right if way == 1 else left
                remote(block, block, send_sem.at[a, k], recv_sem.at[s - 1, a, k], device).wait()

                @pl.when(s < n - 1)
                def _():
                    remote(
                        block, block, send_sem.at[a, k], recv_sem.at[s, a, k], device
                    ).start()

                if extra is not None:

                    @pl.when(s > 1)
                    def _():
                        remote(
                            block,
                            block,
                            xsend_sem.at[a, extra],
                            xrecv_sem.at[s - 1, a, extra],
                            across,
                        ).wait_send()

                    remote(
                        block,
                        block,
                        xsend_sem.at[a, extra],
                        xrecv_sem.at[s - 1, a, extra],
                        across,
                    ).start()
        return 0

    lax.fori_loop(1, n, step, 0)
    if shared:
        for a in range(count):
            for extra in range(2):
                block = outs[a].at[me, extra]
                remote(
                    block, block, xsend_sem.at[a, extra], xrecv_sem.at[0, a, extra], across
                ).wait_send()

        def close(s, _):
            for a in range(count):
                for extra in range(2):
                    way = 1 if extra == 0 else -1
                    owner = ring_index(place + (n - s if way == 1 else s), n)
                    block = outs[a].at[owner, (1 - rep) * 2 + extra]
                    remote(
                        block,
                        block,
                        xsend_sem.at[a, extra],
                        xrecv_sem.at[s - 1, a, extra],
                        across,
                    ).wait_recv()
            return 0

        lax.fori_loop(1, n, close, 0)
    for own in owns:
        own.wait()


def ring_gather(arrays, n, shared, identity):
    count = len(arrays)
    lanes = 6 if shared else arrays[0].shape[0]
    dma = pltpu.SemaphoreType.DMA
    return pl.pallas_call(
        functools.partial(ring_gather_kernel, n, count, shared),
        out_shape=[jax.ShapeDtypeStruct((n,) + a.shape, a.dtype) for a in arrays],
        in_specs=[pl.BlockSpec(memory_space=pltpu.VMEM)] * count,
        out_specs=[pl.BlockSpec(memory_space=pl.ANY)] * count,
        scratch_shapes=[
            dma((count,)),
            dma((count, lanes)),
            dma((n - 1, count, lanes)),
            dma((count, 2)),
            dma((n - 1, count, 2)),
        ],
        compiler_params=pltpu.CompilerParams(collective_id=identity, has_side_effects=True),
    )(*arrays)


def spread_kernel(n, count, *refs):
    ins, outs = refs[:count], refs[count : 2 * count]
    own_sem, send_sem, recv_sem, xsend_sem, xrecv_sem = refs[2 * count :]
    me = lax.axis_index("fs")
    rep = lax.axis_index("rep")
    across = {"rep": 1 - rep}
    greet([{"fs": (me + d) % n} for d in range(1, n)] + [across])
    owns = [
        pltpu.make_async_copy(ins[a].at[me], outs[a].at[me], own_sem.at[a]) for a in range(count)
    ]
    for own in owns:
        own.start()

    def sending(d, a):
        peer = (me + d) % n
        return remote(
            ins[a].at[peer, rep],
            outs[a].at[me, rep],
            send_sem.at[a, d - 1],
            recv_sem.at[a, d - 1],
            {"fs": peer},
        )

    def crossing(d, a, half):
        block = outs[a].at[(me + n - d) % n, half]
        return remote(block, block, xsend_sem.at[a, d - 1], xrecv_sem.at[a, d - 1], across)

    def begin(d, _):
        for a in range(count):
            sending(d, a).start()
        return 0

    def relay(d, _):
        for a in range(count):
            block = outs[a].at[(me + n - d) % n, rep]
            remote(
                block,
                block,
                send_sem.at[a, d - 1],
                recv_sem.at[a, d - 1],
                {"fs": (me + d) % n},
            ).wait_recv()
            crossing(d, a, rep).start()
        return 0

    def close(d, _):
        for a in range(count):
            sending(d, a).wait_send()
            crossing(d, a, rep).wait_send()
            crossing(d, a, 1 - rep).wait_recv()
        return 0

    lax.fori_loop(1, n, begin, 0)
    lax.fori_loop(1, n, relay, 0)
    lax.fori_loop(1, n, close, 0)
    for own in owns:
        own.wait()


def spread(arrays, n, identity):
    count = len(arrays)
    dma = pltpu.SemaphoreType.DMA
    return pl.pallas_call(
        functools.partial(spread_kernel, n, count),
        out_shape=[jax.ShapeDtypeStruct(a.shape, a.dtype) for a in arrays],
        in_specs=[pl.BlockSpec(memory_space=pltpu.VMEM)] * count,
        out_specs=[pl.BlockSpec(memory_space=pl.ANY)] * count,
        scratch_shapes=[dma((count,))] + [dma((count, n - 1)) for _ in range(4)],
        compiler_params=pltpu.CompilerParams(collective_id=identity, has_side_effects=True),
    )(*arrays)


def ring_sum_kernel(n, in_ref, out_ref, held, send_sem, recv_sem):
    me = lax.axis_index("fs")
    place = ring_place(me, n)
    right = {"fs": ring_index(place + 1, n)}
    left = {"fs": ring_index(place + n - 1, n)}
    greet([right, left])
    pieces = in_ref.shape[1]

    def hop(s, k, source):
        return remote(
            source,
            held.at[s, k],
            send_sem.at[s, k],
            recv_sem.at[s, k],
            right if k % 2 == 0 else left,
        )

    def owner(s, k):
        return ring_index(place + (2 * n - 1 - s if k % 2 == 0 else 1 + s), n)

    for k in range(pieces):
        hop(0, k, in_ref.at[owner(0, k), k]).start()

    def step(s, _):
        for k in range(pieces):
            hop(s - 1, k, held.at[s - 1, k]).wait_recv()
            total = held[s - 1, k].astype(jnp.float32) + in_ref[owner(s, k), k].astype(jnp.float32)
            held[s - 1, k] = total.astype(jnp.bfloat16)
            hop(s, k, held.at[s - 1, k]).start()
        return 0

    lax.fori_loop(1, n - 1, step, 0)
    for k in range(pieces):
        hop(n - 2, k, held.at[n - 2, k]).wait_recv()
        out_ref[k] = held[n - 2, k].astype(jnp.float32) + in_ref[me, k].astype(jnp.float32)

    def close(s, _):
        for k in range(pieces):
            hop(s, k, held.at[s, k]).wait_send()
        return 0

    lax.fori_loop(0, n - 1, close, 0)


def ring_sum(shares, n, identity):
    dma = pltpu.SemaphoreType.DMA
    return pl.pallas_call(
        functools.partial(ring_sum_kernel, n),
        out_shape=jax.ShapeDtypeStruct(shares.shape[1:], jnp.float32),
        in_specs=[pl.BlockSpec(memory_space=pltpu.VMEM)],
        out_specs=pl.BlockSpec(memory_space=pltpu.VMEM),
        scratch_shapes=[
            pltpu.VMEM((n - 1,) + shares.shape[1:], shares.dtype),
            dma((n - 1, shares.shape[1])),
            dma((n - 1, shares.shape[1])),
        ],
        compiler_params=pltpu.CompilerParams(collective_id=identity, has_side_effects=True),
    )(shares)


def norm_half(rows, gain):
    wide = rows.astype(jnp.float32)
    total = lax.psum(jnp.sum(wide * wide, axis=1, keepdims=True), "tp")
    width = rows.shape[1]
    parts = lax.axis_size("tp")
    mine = lax.dynamic_slice(gain, (lax.axis_index("tp") * width,), (width,))
    scaled = wide * lax.rsqrt(total / (width * parts) + epsilon) * mine
    return scaled.astype(jnp.bfloat16)


def tp_columns(rows):
    return lax.all_gather(rows, "tp", axis=1, tiled=True)


def heads_of(normed, weight, scale):
    return jnp.dot(normed, weight, preferred_element_type=jnp.float32) * scale


def mixer(activations, mix_gain, four, four_scale, out_full, out_columns, log_decay):
    normed = tp_columns(norm_half(activations, mix_gain))
    total_rows = normed.shape[0]
    sequences = total_rows // LENGTH
    heads = log_decay.shape[0]
    joined = heads_of(normed, four, four_scale)
    unit = joined.shape[1] // 6
    query = joined[:, :unit]
    key_rows = joined[:, unit : 2 * unit]
    value = joined[:, 2 * unit : 4 * unit]
    gate = joined[:, 4 * unit :]
    positions = jnp.arange(LENGTH, dtype=jnp.float32)
    query_heads = rotate(query.reshape(sequences, LENGTH, heads, -1), positions)
    key_heads = rotate(key_rows.reshape(sequences, LENGTH, heads, -1), positions)
    value_heads = value.reshape(sequences, LENGTH, heads, -1)
    retained = retain(query_heads, key_heads, value_heads, log_decay)
    retained = retained * lax.rsqrt(jnp.mean(retained * retained, axis=-1, keepdims=True) + epsilon)
    attended = (retained.reshape(total_rows, -1) * jax.nn.silu(gate)).astype(jnp.bfloat16)
    partial_value = jnp.einsum(
        "rk,jkc->rjc", attended, out_full, preferred_element_type=jnp.float32
    ).reshape(total_rows, -1)
    partial_value = (partial_value * out_columns).astype(jnp.bfloat16)
    mixed = tp_sum(partial_value)
    return (activations.astype(jnp.float32) + mixed).astype(jnp.bfloat16)


def tp_sum(partial_value):
    parts = lax.axis_size("tp")
    width = partial_value.shape[1] // parts
    spread = jnp.moveaxis(partial_value.reshape(-1, parts, width), 1, 0)
    arrived = lax.all_to_all(spread, "tp", 0, 0, tiled=True)
    return jnp.sum(arrived.astype(jnp.float32), axis=0)


def on_device(
    activations,
    mix_gain,
    mlp_gain,
    query_weight,
    query_scale,
    key_weight,
    key_scale,
    value_weight,
    value_scale,
    gate_weight,
    gate_scale,
    out_weight,
    out_scale,
    up_weight,
    up_scale,
    down_weight,
    down_scale,
    log_decay,
):
    bf = jnp.bfloat16
    four_weight = jnp.concatenate(
        [query_weight, key_weight, value_weight, gate_weight], axis=1
    ).astype(bf)
    four_scale = jnp.concatenate([query_scale, key_scale, value_scale, gate_scale])
    n = lax.axis_size("fs")
    out_half = out_weight.astype(bf)
    spare = jnp.stack([out_scale, down_scale])
    four, out_full, scales = ring_gather(
        [
            four_weight.reshape(8, -1, four_weight.shape[1]),
            out_half.reshape(8, -1, out_half.shape[1]),
            jnp.broadcast_to(spare, (8,) + spare.shape),
        ],
        n,
        True,
        0,
    )
    four = four.reshape(-1, four_weight.shape[1])
    out_full = out_full.reshape((n,) + out_half.shape)
    scales = jnp.moveaxis(scales[:, 0], 1, 0).reshape(2, -1)
    depth = up_weight.shape[0]
    up_cut = jnp.moveaxis(up_weight.astype(bf).reshape(depth, n, -1), 1, 0)
    down_cut = down_weight.astype(bf).reshape(n, 2, -1, down_weight.shape[1])
    up_mine, down_mine = spread(
        [up_cut.reshape(n, 2, depth // 2, -1), down_cut], n, 1
    )
    up_mine = up_mine.reshape(n * depth, -1)
    down_mine = down_mine.reshape(n, -1, down_weight.shape[1])
    units = up_mine.shape[1]
    up_columns = lax.dynamic_slice(up_scale, (lax.axis_index("fs") * units,), (units,))
    first = mixer(activations, mix_gain, four, four_scale, out_full, scales[0], log_decay)
    half_rows = norm_half(first, mlp_gain)
    normed_two = tp_columns(
        ring_gather([half_rows.reshape(4, -1, half_rows.shape[1])], n, False, 2)[0].reshape(
            -1, half_rows.shape[1]
        )
    )
    raised = jnp.dot(normed_two, up_mine, preferred_element_type=jnp.float32) * up_columns
    hidden = jnp.square(jax.nn.relu(raised)).astype(bf)
    share = jnp.einsum("ru,jud->rjd", hidden, down_mine, preferred_element_type=jnp.float32)
    share = share.reshape(share.shape[0], -1) * scales[1]
    pair = tp_sum(share.astype(bf)).astype(bf)
    shares = pair.reshape(n, 4, -1, first.shape[1])
    channel = ring_sum(shares, n, 3).reshape(first.shape)
    return (first.astype(jnp.float32) + channel).astype(bf)


def solution(mesh):
    placed = (
        P(("rep", "fs"), "tp"),
        P(),
        P(),
        P("fs", "tp"),
        P("tp"),
        P("fs", "tp"),
        P("tp"),
        P("fs", "tp"),
        P("tp"),
        P("fs", "tp"),
        P("tp"),
        P("tp", "fs"),
        P("fs"),
        P("fs", "tp"),
        P("tp"),
        P("tp", "fs"),
        P("fs"),
        P("tp"),
    )
    return jax.shard_map(
        on_device, mesh=mesh, in_specs=placed, out_specs=P(("rep", "fs"), "tp"), check_vma=False
    )
```

```python
import functools

import jax
import jax.numpy as jnp
from jax import lax
from jax.experimental import pallas as pl
from jax.experimental.pallas import tpu as pltpu
from jax.sharding import PartitionSpec as P

BLOCK = 64
LENGTH = 192


epsilon = 1e-06
rope_base = 10000.0


def rotate(head_rows, positions):
    half = head_rows.shape[-1] // 2
    inverse = 1.0 / rope_base ** jnp.linspace(0.0, 1.0, half, dtype=jnp.float32)
    angles = positions[:, None] * inverse[None, :]
    cosine = jnp.cos(angles)[:, None, :]
    sine = jnp.sin(angles)[:, None, :]
    first = head_rows[..., :half]
    second = head_rows[..., half:]
    return jnp.concatenate(
        [first * cosine - second * sine, first * sine + second * cosine], axis=-1
    )


def retain(query_heads, key_heads, value_heads, log_decay):
    batch, length, heads, width = query_heads.shape
    block_count = length // BLOCK
    highest = lax.Precision.HIGHEST

    def to_blocks(tensor):
        return tensor.reshape(batch, block_count, BLOCK, heads, tensor.shape[-1]).transpose(
            0, 3, 1, 2, 4
        )

    query_blocks = to_blocks(query_heads)
    key_blocks = to_blocks(key_heads)
    value_blocks = to_blocks(value_heads)
    places = jnp.arange(BLOCK, dtype=jnp.float32)
    offsets = places[:, None] - places[None, :]
    inner = jnp.where(
        offsets >= 0, jnp.exp(log_decay[:, None, None] * jnp.maximum(offsets, 0.0)), 0.0
    )
    scores = (
        jnp.einsum("bhntd,bhnsd->bhnts", query_blocks, key_blocks, precision=highest)
        * inner[None, :, None]
    )
    output = jnp.einsum("bhnts,bhnse->bhnte", scores, value_blocks, precision=highest)
    keys_decayed = (
        key_blocks
        * jnp.exp(log_decay[:, None] * (BLOCK - 1.0 - places)[None, :])[None, :, None, :, None]
    )
    increments = jnp.einsum("bhnsd,bhnse->nbhde", keys_decayed, value_blocks, precision=highest)
    carry_decay = jnp.exp(log_decay * BLOCK)[None, :, None, None]

    def advance(state, increment):
        return (carry_decay * state + increment, state)

    initial = jnp.zeros((batch, heads, width, value_heads.shape[-1]), jnp.float32)
    _, states = lax.scan(advance, initial, increments)
    query_decayed = (
        query_blocks * jnp.exp(log_decay[:, None] * (places + 1.0)[None, :])[None, :, None, :, None]
    )
    output = output + jnp.einsum("bhntd,nbhde->bhnte", query_decayed, states, precision=highest)
    return output.transpose(0, 2, 3, 1, 4).reshape(batch, length, heads, value_heads.shape[-1])


MESH = pl.DeviceIdType.MESH


def ring_place(index, n):
    odd = index % 2
    return (1 - odd) * (index // 2) + odd * (n - 1 - index // 2)


def ring_index(place, n):
    place = (place + n) % n
    late = (2 * place) // n
    return (1 - late) * (2 * place) + late * (2 * (n - 1 - place) + 1)


def greet(targets):
    barrier = pltpu.get_barrier_semaphore()
    for target in targets:
        pl.semaphore_signal(barrier, inc=1, device_id=target, device_id_type=MESH)
    pl.semaphore_wait(barrier, len(targets))


def remote(source, target, send, recv, device):
    return pltpu.make_async_remote_copy(
        src_ref=source,
        dst_ref=target,
        send_sem=send,
        recv_sem=recv,
        device_id=device,
        device_id_type=MESH,
    )


def ring_gather_kernel(n, count, shared, *refs):
    ins, outs = refs[:count], refs[count : 2 * count]
    own_sem, send_sem, recv_sem, xsend_sem, xrecv_sem = refs[2 * count :]
    me = lax.axis_index("fs")
    place = ring_place(me, n)
    chunks = ins[0].shape[0]
    quarter = chunks // 4
    right = {"fs": ring_index(place + 1, n)}
    left = {"fs": ring_index(place + n - 1, n)}
    targets = [right, left]
    if shared:
        rep = lax.axis_index("rep")
        across = {"rep": 1 - rep}
        targets.append(across)
        lanes = [
            (rep * 2, 1, 0),
            (rep * 2 + 1, -1, 1),
            (4, 1, None),
            (6, -1, None),
            (5, 1, None),
            (7, -1, None),
        ]
    else:
        lanes = [(k, 1 if k % 2 == 0 else -1, None) for k in range(chunks)]
    greet(targets)
    owns = [
        pltpu.make_async_copy(ins[a], outs[a].at[me], own_sem.at[a]) for a in range(count)
    ]
    for own in owns:
        own.start()
    for k, (chunk, way, _) in enumerate(lanes):
        for a in range(count):
            remote(
                ins[a].at[chunk],
                outs[a].at[me, chunk],
                send_sem.at[a, k],
                recv_sem.at[0, a, k],
                right if way == 1 else left,
            ).start()

    def step(s, _):
        for k, (chunk, way, extra) in enumerate(lanes):
            owner = ring_index(place + (n - s if way == 1 else s), n)
            for a in range(count):
                block = outs[a].at[owner, chunk]
                device = right if way == 1 else left
                remote(block, block, send_sem.at[a, k], recv_sem.at[s - 1, a, k], device).wait()

                @pl.when(s < n - 1)
                def _():
                    remote(
                        block, block, send_sem.at[a, k], recv_sem.at[s, a, k], device
                    ).start()

                if extra is not None:

                    @pl.when(s > 1)
                    def _():
                        remote(
                            block,
                            block,
                            xsend_sem.at[a, extra],
                            xrecv_sem.at[s - 1, a, extra],
                            across,
                        ).wait_send()

                    remote(
                        block,
                        block,
                        xsend_sem.at[a, extra],
                        xrecv_sem.at[s - 1, a, extra],
                        across,
                    ).start()
        return 0

    lax.fori_loop(1, n, step, 0)
    if shared:
        for a in range(count):
            for extra in range(2):
                block = outs[a].at[me, extra]
                remote(
                    block, block, xsend_sem.at[a, extra], xrecv_sem.at[0, a, extra], across
                ).wait_send()

        def close(s, _):
            for a in range(count):
                for extra in range(2):
                    way = 1 if extra == 0 else -1
                    owner = ring_index(place + (n - s if way == 1 else s), n)
                    block = outs[a].at[owner, (1 - rep) * 2 + extra]
                    remote(
                        block,
                        block,
                        xsend_sem.at[a, extra],
                        xrecv_sem.at[s - 1, a, extra],
                        across,
                    ).wait_recv()
            return 0

        lax.fori_loop(1, n, close, 0)
    for own in owns:
        own.wait()


def ring_gather(arrays, n, shared, identity):
    count = len(arrays)
    lanes = 6 if shared else arrays[0].shape[0]
    dma = pltpu.SemaphoreType.DMA
    return pl.pallas_call(
        functools.partial(ring_gather_kernel, n, count, shared),
        out_shape=[jax.ShapeDtypeStruct((n,) + a.shape, a.dtype) for a in arrays],
        in_specs=[pl.BlockSpec(memory_space=pltpu.VMEM)] * count,
        out_specs=[pl.BlockSpec(memory_space=pl.ANY)] * count,
        scratch_shapes=[
            dma((count,)),
            dma((count, lanes)),
            dma((n - 1, count, lanes)),
            dma((count, 2)),
            dma((n - 1, count, 2)),
        ],
        compiler_params=pltpu.CompilerParams(collective_id=identity, has_side_effects=True),
    )(*arrays)


def spread_kernel(n, count, *refs):
    ins, outs = refs[:count], refs[count : 2 * count]
    own_sem, send_sem, recv_sem, xsend_sem, xrecv_sem = refs[2 * count :]
    me = lax.axis_index("fs")
    rep = lax.axis_index("rep")
    across = {"rep": 1 - rep}
    greet([{"fs": (me + d) % n} for d in range(1, n)] + [across])
    owns = [
        pltpu.make_async_copy(ins[a].at[me], outs[a].at[me], own_sem.at[a]) for a in range(count)
    ]
    for own in owns:
        own.start()

    def sending(d, a):
        peer = (me + d) % n
        return remote(
            ins[a].at[peer, rep],
            outs[a].at[me, rep],
            send_sem.at[a, d - 1],
            recv_sem.at[a, d - 1],
            {"fs": peer},
        )

    def crossing(d, a, half):
        block = outs[a].at[(me + n - d) % n, half]
        return remote(block, block, xsend_sem.at[a, d - 1], xrecv_sem.at[a, d - 1], across)

    def begin(d, _):
        for a in range(count):
            sending(d, a).start()
        return 0

    def relay(d, _):
        for a in range(count):
            block = outs[a].at[(me + n - d) % n, rep]
            remote(
                block,
                block,
                send_sem.at[a, d - 1],
                recv_sem.at[a, d - 1],
                {"fs": (me + d) % n},
            ).wait_recv()
            crossing(d, a, rep).start()
        return 0

    def close(d, _):
        for a in range(count):
            sending(d, a).wait_send()
            crossing(d, a, rep).wait_send()
            crossing(d, a, 1 - rep).wait_recv()
        return 0

    lax.fori_loop(1, n, begin, 0)
    lax.fori_loop(1, n, relay, 0)
    lax.fori_loop(1, n, close, 0)
    for own in owns:
        own.wait()


def spread(arrays, n, identity):
    count = len(arrays)
    dma = pltpu.SemaphoreType.DMA
    return pl.pallas_call(
        functools.partial(spread_kernel, n, count),
        out_shape=[jax.ShapeDtypeStruct(a.shape, a.dtype) for a in arrays],
        in_specs=[pl.BlockSpec(memory_space=pltpu.VMEM)] * count,
        out_specs=[pl.BlockSpec(memory_space=pl.ANY)] * count,
        scratch_shapes=[dma((count,))] + [dma((count, n - 1)) for _ in range(4)],
        compiler_params=pltpu.CompilerParams(collective_id=identity, has_side_effects=True),
    )(*arrays)


def ring_sum_kernel(n, in_ref, out_ref, held, send_sem, recv_sem):
    me = lax.axis_index("fs")
    place = ring_place(me, n)
    right = {"fs": ring_index(place + 1, n)}
    left = {"fs": ring_index(place + n - 1, n)}
    greet([right, left])
    pieces = in_ref.shape[1]

    def hop(s, k, source):
        return remote(
            source,
            held.at[s, k],
            send_sem.at[s, k],
            recv_sem.at[s, k],
            right if k % 2 == 0 else left,
        )

    def owner(s, k):
        return ring_index(place + (2 * n - 1 - s if k % 2 == 0 else 1 + s), n)

    for k in range(pieces):
        hop(0, k, in_ref.at[owner(0, k), k]).start()

    def step(s, _):
        for k in range(pieces):
            hop(s - 1, k, held.at[s - 1, k]).wait_recv()
            total = held[s - 1, k].astype(jnp.float32) + in_ref[owner(s, k), k].astype(jnp.float32)
            held[s - 1, k] = total.astype(jnp.bfloat16)
            hop(s, k, held.at[s - 1, k]).start()
        return 0

    lax.fori_loop(1, n - 1, step, 0)
    for k in range(pieces):
        hop(n - 2, k, held.at[n - 2, k]).wait_recv()
        out_ref[k] = held[n - 2, k].astype(jnp.float32) + in_ref[me, k].astype(jnp.float32)

    def close(s, _):
        for k in range(pieces):
            hop(s, k, held.at[s, k]).wait_send()
        return 0

    lax.fori_loop(0, n - 1, close, 0)


def ring_sum(shares, n, identity):
    dma = pltpu.SemaphoreType.DMA
    return pl.pallas_call(
        functools.partial(ring_sum_kernel, n),
        out_shape=jax.ShapeDtypeStruct(shares.shape[1:], jnp.float32),
        in_specs=[pl.BlockSpec(memory_space=pltpu.VMEM)],
        out_specs=pl.BlockSpec(memory_space=pltpu.VMEM),
        scratch_shapes=[
            pltpu.VMEM((n - 1,) + shares.shape[1:], shares.dtype),
            dma((n - 1, shares.shape[1])),
            dma((n - 1, shares.shape[1])),
        ],
        compiler_params=pltpu.CompilerParams(collective_id=identity, has_side_effects=True),
    )(shares)


def norm_half(rows, gain):
    wide = rows.astype(jnp.float32)
    total = lax.psum(jnp.sum(wide * wide, axis=1, keepdims=True), "tp")
    width = rows.shape[1]
    parts = lax.axis_size("tp")
    mine = lax.dynamic_slice(gain, (lax.axis_index("tp") * width,), (width,))
    scaled = wide * lax.rsqrt(total / (width * parts) + epsilon) * mine
    return scaled.astype(jnp.bfloat16)


def tp_columns(rows):
    return lax.all_gather(rows, "tp", axis=1, tiled=True)


def heads_of(normed, weight, scale):
    return jnp.dot(normed, weight, preferred_element_type=jnp.float32) * scale


def mixer(activations, mix_gain, four, four_scale, out_full, out_columns, log_decay):
    normed = tp_columns(norm_half(activations, mix_gain))
    total_rows = normed.shape[0]
    sequences = total_rows // LENGTH
    heads = log_decay.shape[0]
    joined = heads_of(normed, four, four_scale)
    unit = joined.shape[1] // 6
    query = joined[:, :unit]
    key_rows = joined[:, unit : 2 * unit]
    value = joined[:, 2 * unit : 4 * unit]
    gate = joined[:, 4 * unit :]
    positions = jnp.arange(LENGTH, dtype=jnp.float32)
    query_heads = rotate(query.reshape(sequences, LENGTH, heads, -1), positions)
    key_heads = rotate(key_rows.reshape(sequences, LENGTH, heads, -1), positions)
    value_heads = value.reshape(sequences, LENGTH, heads, -1)
    retained = retain(query_heads, key_heads, value_heads, log_decay)
    retained = retained * lax.rsqrt(jnp.mean(retained * retained, axis=-1, keepdims=True) + epsilon)
    attended = (retained.reshape(total_rows, -1) * jax.nn.silu(gate)).astype(jnp.bfloat16)
    partial_value = jnp.einsum(
        "rk,jkc->rjc", attended, out_full, preferred_element_type=jnp.float32
    ).reshape(total_rows, -1)
    partial_value = (partial_value * out_columns).astype(jnp.bfloat16)
    mixed = tp_sum(partial_value)
    return (activations.astype(jnp.float32) + mixed).astype(jnp.bfloat16)


def tp_sum(partial_value):
    parts = lax.axis_size("tp")
    width = partial_value.shape[1] // parts
    spread = jnp.moveaxis(partial_value.reshape(-1, parts, width), 1, 0)
    arrived = lax.all_to_all(spread, "tp", 0, 0, tiled=True)
    return jnp.sum(arrived.astype(jnp.float32), axis=0)


def on_device(
    activations,
    mix_gain,
    mlp_gain,
    query_weight,
    query_scale,
    key_weight,
    key_scale,
    value_weight,
    value_scale,
    gate_weight,
    gate_scale,
    out_weight,
    out_scale,
    up_weight,
    up_scale,
    down_weight,
    down_scale,
    log_decay,
):
    bf = jnp.bfloat16
    four_weight = jnp.concatenate(
        [query_weight, key_weight, value_weight, gate_weight], axis=1
    ).astype(bf)
    four_scale = jnp.concatenate([query_scale, key_scale, value_scale, gate_scale])
    n = lax.axis_size("fs")
    out_half = out_weight.astype(bf)
    spare = jnp.stack([out_scale, down_scale])
    four, out_full, scales = ring_gather(
        [
            four_weight.reshape(8, -1, four_weight.shape[1]),
            out_half.reshape(8, -1, out_half.shape[1]),
            jnp.broadcast_to(spare, (8,) + spare.shape),
        ],
        n,
        True,
        0,
    )
    four = four.reshape(-1, four_weight.shape[1])
    out_full = out_full.reshape((n,) + out_half.shape)
    scales = jnp.moveaxis(scales[:, 0], 1, 0).reshape(2, -1)
    depth = up_weight.shape[0]
    up_cut = jnp.moveaxis(up_weight.astype(bf).reshape(depth, n, -1), 1, 0)
    down_cut = down_weight.astype(bf).reshape(n, 2, -1, down_weight.shape[1])
    up_mine, down_mine = spread(
        [up_cut.reshape(n, 2, depth // 2, -1), down_cut], n, 1
    )
    up_mine = up_mine.reshape(n * depth, -1)
    down_mine = down_mine.reshape(n, -1, down_weight.shape[1])
    units = up_mine.shape[1]
    up_columns = lax.dynamic_slice(up_scale, (lax.axis_index("fs") * units,), (units,))
    first = mixer(activations, mix_gain, four, four_scale, out_full, scales[0], log_decay)
    half_rows = norm_half(first, mlp_gain)
    normed_two = tp_columns(
        ring_gather([half_rows.reshape(6, -1, half_rows.shape[1])], n, False, 2)[0].reshape(
            -1, half_rows.shape[1]
        )
    )
    raised = jnp.dot(normed_two, up_mine, preferred_element_type=jnp.float32) * up_columns
    hidden = jnp.square(jax.nn.relu(raised)).astype(bf)
    share = jnp.einsum("ru,jud->rjd", hidden, down_mine, preferred_element_type=jnp.float32)
    share = share.reshape(share.shape[0], -1) * scales[1]
    pair = tp_sum(share.astype(bf)).astype(bf)
    shares = pair.reshape(n, 12, -1, first.shape[1])
    channel = ring_sum(shares, n, 3).reshape(first.shape)
    return (first.astype(jnp.float32) + channel).astype(bf)


def solution(mesh):
    placed = (
        P(("rep", "fs"), "tp"),
        P(),
        P(),
        P("fs", "tp"),
        P("tp"),
        P("fs", "tp"),
        P("tp"),
        P("fs", "tp"),
        P("tp"),
        P("fs", "tp"),
        P("tp"),
        P("tp", "fs"),
        P("fs"),
        P("fs", "tp"),
        P("tp"),
        P("tp", "fs"),
        P("fs"),
        P("tp"),
    )
    return jax.shard_map(
        on_device, mesh=mesh, in_specs=placed, out_specs=P(("rep", "fs"), "tp"), check_vma=False
    )
```
